32 devices in a mesh: kv: 8 (over z, y), tp: 4 (over x, core).
Axes of the slice: x: 2, y: 2, z: 4, core: 2. Of those that a mesh axis runs over, the one named last changes fastest.
Arguments:
- tokens: bfloat16 [16, 16, 4096], replicated, may hold values from -6 to 6
- gain_pre: float32 [4096], replicated, may hold values from 0.1 to 1.9
- w_query: bfloat16 [4096, 2048], P('kv', 'tp'), may hold values from -0.09375 to 0.09375
- w_key: bfloat16 [4096, 2048], P('kv', 'tp'), may hold values from -0.09375 to 0.09375
- w_value: bfloat16 [4096, 2048], P('kv', 'tp'), may hold values from -0.09375 to 0.09375
- w_forget: bfloat16 [4096, 16], replicated, may hold values from -0.09375 to 0.09375
- b_forget: float32 [16], replicated
- w_out: bfloat16 [2048, 4096], P('tp', 'kv'), may hold values from -0.125 to 0.125
- gain_post: float32 [4096], P(('kv', 'tp')), may hold values from 0.1 to 1.9
- key_cache: bfloat16 [16, 1024, 16, 128], P(None, 'kv', 'tp'), may hold values from -6 to 6
- value_cache: bfloat16 [16, 1024, 16, 128], P(None, 'kv', 'tp'), may hold values from -6 to 6
- cum_cache: float32 [16, 1024, 16], P(None, 'kv', 'tp'), may hold values from -402 to 0, as said below
- lengths: int32 [16], replicated, may hold values from 512 to 992
- accepted: int32 [16], replicated, may hold values from 0 to 16
- parent: int32 [16, 16], replicated, may hold values from -1 to 14, as said below
Outputs:
- mixed: bfloat16 [16, 16, 4096], P(None, None, ('kv', 'tp'))
- key_out: bfloat16 [16, 1024, 16, 128], P(None, 'kv', 'tp')
- value_out: bfloat16 [16, 1024, 16, 128], P(None, 'kv', 'tp')
- cum_out: float32 [16, 1024, 16], P(None, 'kv', 'tp')
The draws below stay inside these ranges and needn't reach their ends.
Inputs may be any that keep to these rules, and one draw needn't show every extreme that they name: parent[s, 0] is -1 and parent[s, i] lies between -1 and i - 1. `cum_cache`: along the positions of each sequence and head the values never rise. lengths + accepted + 16 never exceeds 1024.
All inputs are finite; a program needn't handle non-finite values.
Results may differ from the reference program's by a relative error of at most 0.03.
Values may be sent and summed in bfloat16 or wider, within the bound.
No kernel may reach another device: no remote copies, remote signals or barrier semaphores. Data moves between devices by JAX's collectives and lax.ppermute only.
A program may use at most 64 MiB of HBM per device.

```python
import jax
import jax.numpy as jnp
from jax import lax

D = 4096
HEADS = 16
HD = 128
PROP = 16
SEQS = 16
POS_DEV = 128
HW = 2048
CACHE_LEN = 1024
SHARDS = 8
GROUPS = 4


def fast_heads(key):
    share = 0.5
    return jax.random.bernoulli(jax.random.fold_in(key, 11), share, (HEADS,))


def draw_b_forget(key, part):
    fast = fast_heads(key)
    spread = jax.random.uniform(jax.random.fold_in(key, 12), (HEADS,), jnp.float32)
    return jnp.where(fast, 0.5 + 1.5 * spread, 2.5 + 1.5 * spread).astype(jnp.float32)


def draw_cum_cache(key, part):
    fast = fast_heads(key)
    slow_rate = jax.random.uniform(jax.random.fold_in(key, 21), (SEQS, HEADS), jnp.float32, 0.3, 1.2) / CACHE_LEN
    fast_rate = 1.0 / jax.random.uniform(jax.random.fold_in(key, 22), (SEQS, HEADS), jnp.float32, 40.0, 100.0)
    rates = jnp.where(fast[None, :], fast_rate, slow_rate)
    factor_pos = jnp.exp(jax.random.uniform(jax.random.fold_in(key, 23), (SEQS, CACHE_LEN, HEADS), jnp.float32, jnp.log(0.6), jnp.log(1.6)))
    factor_block = jnp.exp(jax.random.uniform(jax.random.fold_in(key, 24), (SEQS, CACHE_LEN // POS_DEV, HEADS), jnp.float32, jnp.log(0.5), jnp.log(2.0)))
    factor_block = jnp.repeat(factor_block, POS_DEV, axis=1)
    decrements = -rates[:, None, :] * factor_pos * factor_block
    offsets = jax.random.uniform(jax.random.fold_in(key, 25), (SEQS, 1, HEADS), jnp.float32, -300.0, 0.0)
    return (offsets + jnp.cumsum(decrements, axis=1)).astype(jnp.float32)


def draw_parent(key, part):
    limits = jnp.arange(PROP, dtype=jnp.int32)[None, :]
    return jax.random.randint(key, (SEQS, PROP), -1, limits, dtype=jnp.int32)


def place_ends(entries, stream_key, least, largest):
    longest = entries.shape.index(max(entries.shape))
    spots = []
    for shift in (0, 1):
        where = [jax.random.randint(jax.random.fold_in(stream_key, axis), (), 0, length) for axis, length in enumerate(entries.shape)]
        where[longest] = (where[longest] + shift) % entries.shape[longest]
        spots.append(tuple(where))
    return entries.at[spots[0]].set(least).at[spots[1]].set(largest)


def shard_levels(key, extent, split, low, largest):
    def one(position, blocks):
        draws = jax.random.uniform(jax.random.fold_in(jax.random.fold_in(key, 6), position), (blocks,), jnp.float32, low / len(split), largest / len(split))
        return jnp.repeat(jnp.exp(draws), extent[position] // blocks).reshape((-1,) + (1,) * (len(extent) - position - 1))

    factor_of = one(*split[0])
    for cut in split[1:]:
        factor_of = factor_of * one(*cut)
    return factor_of


def normal_values(key, shape, width, most, split=(), kind=jnp.bfloat16):
    gain = shard_levels(key, shape, split, -0.22, 0.18) if split else 1.0
    drawn = jax.random.normal(key, shape, jnp.float32) * width * gain
    return jnp.minimum(jnp.maximum(drawn, -most), most).astype(kind)


def setup_inputs(seed: int = 0) -> dict:
    key_of = jax.random.split(jax.random.key(seed), 16)
    tokens = normal_values(key_of[0], (SEQS, PROP, D), 1.0, 6.0)
    gain_pre = jnp.clip(1.0 + 0.18 * jax.random.normal(key_of[1], (D,), jnp.float32), 0.1, 1.9)
    w_query = normal_values(key_of[2], (D, HW), D ** -0.5, 0.09375, ((0, 8), (1, 4)))
    w_key = normal_values(key_of[3], (D, HW), D ** -0.5, 0.09375, ((0, 8), (1, 4)))
    w_value = normal_values(key_of[4], (D, HW), D ** -0.5, 0.09375, ((0, 8), (1, 4)))
    w_forget = normal_values(key_of[5], (D, HEADS), D ** -0.5, 0.09375)
    b_forget = draw_b_forget(jax.random.fold_in(key_of[15], 71), 0)
    w_out = normal_values(key_of[7], (HW, D), HW ** -0.5, 0.125, ((0, 4), (1, 8)))
    gain_post = jnp.clip(1.0 + 0.18 * jax.random.normal(key_of[8], (D,), jnp.float32), 0.1, 1.9)
    key_cache = normal_values(key_of[9], (SEQS, CACHE_LEN, HEADS, HD), 1.0, 6.0, ((1, 8), (2, 4)))
    value_cache = normal_values(key_of[10], (SEQS, CACHE_LEN, HEADS, HD), 1.0, 6.0, ((1, 8), (2, 4)))
    cum_cache = draw_cum_cache(jax.random.fold_in(key_of[15], 71), 0)
    lengths = place_ends(jax.random.randint(key_of[12], (SEQS,), CACHE_LEN // 2, CACHE_LEN - 2 * PROP + 1), jax.random.fold_in(key_of[12], 1), CACHE_LEN // 2, CACHE_LEN - 2 * PROP).astype(jnp.int32)
    accepted = place_ends(jax.random.randint(key_of[13], (SEQS,), 0, PROP + 1), jax.random.fold_in(key_of[13], 1), 0, PROP).astype(jnp.int32)
    parent = draw_parent(jax.random.fold_in(key_of[15], 71), 0)
    return {"tokens": tokens, "gain_pre": gain_pre, "w_query": w_query, "w_key": w_key, "w_value": w_value, "w_forget": w_forget, "b_forget": b_forget, "w_out": w_out, "gain_post": gain_post, "key_cache": key_cache, "value_cache": value_cache, "cum_cache": cum_cache, "lengths": lengths, "accepted": accepted, "parent": parent}


epsilon = 1e-06
floor_value = -1e+30

def ancestry(parent_ids, members):
    identity = jnp.eye(members, dtype=jnp.float32)
    parent_hot = (parent_ids[:, :, None] == jnp.arange(members, dtype=jnp.int32)[None, None, :]).astype(jnp.float32)
    ancestors = jnp.minimum(identity[None] + parent_hot, 1.0)
    for sweep in range(max(1, (members - 1).bit_length())):
        ancestors = jnp.minimum(jnp.einsum('bij,bjk->bik', ancestors, ancestors, precision=lax.Precision.HIGHEST), 1.0)
    return ancestors

def reference(tokens, gain_pre, w_query, w_key, w_value, w_forget, b_forget, w_out, gain_post, key_cache, value_cache, cum_cache, lengths, accepted, parent):
    num_seqs = tokens.shape[0]
    scale = HD ** (-0.5)
    tok_float = tokens.astype(jnp.float32)
    normed = (tok_float * lax.rsqrt(lax.optimization_barrier(jnp.mean(tok_float * tok_float, -1, keepdims=True)) + epsilon) * gain_pre.astype(jnp.float32)).astype(jnp.bfloat16)
    flat = normed.reshape(num_seqs * PROP, D)
    query = jnp.dot(flat, w_query, preferred_element_type=jnp.float32).astype(jnp.bfloat16).reshape(num_seqs, PROP, HEADS, HD)
    key_new = jnp.dot(flat, w_key, preferred_element_type=jnp.float32).astype(jnp.bfloat16).reshape(num_seqs, PROP, HEADS, HD)
    value_new = jnp.dot(flat, w_value, preferred_element_type=jnp.float32).astype(jnp.bfloat16).reshape(num_seqs, PROP, HEADS, HD)
    log_forget = jax.nn.log_sigmoid(jnp.dot(flat, w_forget, preferred_element_type=jnp.float32) + b_forget.astype(jnp.float32)).reshape(num_seqs, PROP, HEADS)
    ancestors = ancestry(parent, PROP)
    path = jnp.einsum('bij,bjh->bih', ancestors, log_forget, precision=lax.Precision.HIGHEST)
    valid = (lengths + accepted).astype(jnp.int32)
    last_index = jnp.broadcast_to((valid - 1).astype(jnp.int32)[:, None, None], (num_seqs, 1, HEADS))
    last_cum = jnp.take_along_axis(cum_cache, last_index, axis=1)[:, 0, :]
    query_float = query.astype(jnp.float32)
    key_blocks = jnp.swapaxes(key_cache.reshape(num_seqs, SHARDS, POS_DEV, HEADS, HD), 0, 1)
    value_blocks = jnp.swapaxes(value_cache.reshape(num_seqs, SHARDS, POS_DEV, HEADS, HD), 0, 1)
    cum_blocks = jnp.swapaxes(cum_cache.reshape(num_seqs, SHARDS, POS_DEV, HEADS), 0, 1)
    starts = (jnp.arange(SHARDS, dtype=jnp.int32) * POS_DEV).astype(jnp.int32)

    def add_block(carry, item):
        run_max, run_total, run_values = carry
        block_keys, block_vals, block_cum, start = item
        positions = start + jnp.arange(POS_DEV, dtype=jnp.int32)
        live = (positions[None, :] < valid[:, None])[:, None, None, :]
        score = jnp.einsum('bihd,bkhd->bihk', query_float, block_keys.astype(jnp.float32)) * scale + path[..., None] - jnp.swapaxes(block_cum, 1, 2)[:, None]
        block_max = lax.optimization_barrier(jnp.max(jnp.where(live, score, floor_value), axis=-1))
        weight = jnp.exp(jnp.where(live, score - block_max[..., None], floor_value))
        block_total = lax.optimization_barrier(jnp.sum(weight, axis=-1))
        weight_low = lax.optimization_barrier(weight.astype(jnp.bfloat16)).astype(jnp.float32)
        block_values = jnp.einsum('bihk,bkhd->bihd', weight_low, block_vals.astype(jnp.float32))
        new_max = jnp.maximum(run_max, block_max)
        old_scale = jnp.exp(run_max - new_max)
        new_scale = jnp.exp(block_max - new_max)
        return ((new_max, run_total * old_scale + block_total * new_scale, run_values * old_scale[..., None] + block_values * new_scale[..., None]), None)
    init = (jnp.full((num_seqs, PROP, HEADS), floor_value, jnp.float32), jnp.zeros((num_seqs, PROP, HEADS), jnp.float32), jnp.zeros((num_seqs, PROP, HEADS, HD), jnp.float32))
    (cache_max, cache_total, cache_values), unused = lax.scan(add_block, init, (key_blocks, value_blocks, cum_blocks, starts))
    tree_mask = (ancestors > 0.5)[:, :, None, :]
    tree_score = jnp.einsum('bihd,bjhd->bihj', query_float, key_new.astype(jnp.float32)) * scale + path[..., None] - jnp.swapaxes(path, 1, 2)[:, None]
    tree_max = lax.optimization_barrier(jnp.max(jnp.where(tree_mask, tree_score, floor_value), axis=-1))
    tree_weight = jnp.exp(jnp.where(tree_mask, tree_score - tree_max[..., None], floor_value))
    tree_total = lax.optimization_barrier(jnp.sum(tree_weight, axis=-1))
    tree_low = lax.optimization_barrier(tree_weight.astype(jnp.bfloat16)).astype(jnp.float32)
    tree_values = jnp.einsum('bihj,bjhd->bihd', tree_low, value_new.astype(jnp.float32))
    shifted = cache_max + last_cum[:, None, :]
    top = jnp.maximum(shifted, tree_max)
    cache_scale = jnp.exp(shifted - top)
    tree_scale = jnp.exp(tree_max - top)
    attended = ((cache_values * cache_scale[..., None] + tree_values * tree_scale[..., None]) / (cache_total * cache_scale + tree_total * tree_scale)[..., None]).astype(jnp.bfloat16)
    attended = attended.reshape(num_seqs * PROP, GROUPS, HW // GROUPS).astype(jnp.float32)
    group_out = jnp.einsum('tgc,gcd->gtd', attended, w_out.reshape(GROUPS, HW // GROUPS, D).astype(jnp.float32))
    group_out = lax.optimization_barrier(group_out.astype(jnp.bfloat16)).astype(jnp.float32)
    mixed_sum = lax.optimization_barrier(jnp.sum(group_out, axis=0))
    mixed = (mixed_sum * lax.rsqrt(lax.optimization_barrier(jnp.mean(mixed_sum * mixed_sum, -1, keepdims=True)) + epsilon) * gain_post.astype(jnp.float32)).astype(jnp.bfloat16).reshape(num_seqs, PROP, D)
    zero_index = jnp.zeros((), jnp.int32)

    def write_rows(cache_rows, new_rows, start):
        return lax.dynamic_update_slice(cache_rows, new_rows, (start.astype(jnp.int32), zero_index, zero_index))
    key_out = jax.vmap(write_rows)(key_cache, key_new, valid)
    value_out = jax.vmap(write_rows)(value_cache, value_new, valid)
    cum_new = last_cum[:, None, :] + path

    def write_cum(cache_rows, new_rows, start):
        return lax.dynamic_update_slice(cache_rows, new_rows, (start.astype(jnp.int32), zero_index))
    cum_out = jax.vmap(write_cum)(cum_cache, cum_new, valid)
    return (mixed, key_out, value_out, cum_out)
```

```python
import jax
import jax.numpy as jnp
from jax import lax
from jax.sharding import PartitionSpec as P

epsilon = 1e-06
floor_value = -1e30


def split_float(x):
    high = lax.reduce_precision(x, 8, 7)
    rest = x - high
    middle = lax.reduce_precision(rest, 8, 7)
    low = rest - middle
    return [part.astype(jnp.bfloat16) for part in (high, middle, low)]


def pack_lanes(x, lanes):
    parts = jnp.concatenate(split_float(x), axis=-1)
    return jnp.pad(parts, ((0, 0), (0, lanes - parts.shape[-1])))


def unpack_lanes(packed, count):
    wide = packed.astype(jnp.float32)
    return (
        wide[..., :count] + wide[..., count : 2 * count] + wide[..., 2 * count : 3 * count]
    )


def gather_rows(rows, axis):
    size = lax.axis_size(axis)
    copies = jnp.broadcast_to(rows[None], (size,) + rows.shape)
    return lax.all_to_all(copies, axis, 0, 0, tiled=True).reshape(
        (size * rows.shape[0],) + rows.shape[1:]
    )


def exchange(rows, axis):
    size = lax.axis_size(axis)
    blocks = rows.reshape((size, rows.shape[0] // size) + rows.shape[1:])
    return lax.all_to_all(blocks, axis, 0, 0, tiled=True)


def scatter_columns(part, axis):
    size = lax.axis_size(axis)
    rank = lax.axis_index(axis)
    width = part.shape[1] // size
    arrived = [
        lax.ppermute(
            lax.dynamic_slice_in_dim(part, ((rank + step) % size) * width, width, 1),
            axis,
            [(i, (i + step) % size) for i in range(size)],
        )
        for step in range(1, size)
    ]
    total = lax.dynamic_slice_in_dim(part, rank * width, width, 1).astype(jnp.float32)
    for block in arrived:
        total = total + block.astype(jnp.float32)
    return total


def ancestry(parent_ids, members):
    identity = jnp.eye(members, dtype=jnp.float32)
    parent_hot = (
        parent_ids[:, :, None] == jnp.arange(members, dtype=jnp.int32)[None, None, :]
    ).astype(jnp.float32)
    ancestors = jnp.minimum(identity[None] + parent_hot, 1.0)
    for sweep in range(max(1, (members - 1).bit_length())):
        ancestors = jnp.minimum(
            jnp.einsum("bij,bjk->bik", ancestors, ancestors, precision=lax.Precision.HIGHEST), 1.0
        )
    return ancestors


def finish_rows(cache_max, cache_total, cache_values, last_rows, tree_max, tree_total, tree_values):
    shifted = cache_max + last_rows
    top = jnp.maximum(shifted, tree_max)
    cache_scale = jnp.exp(shifted - top)
    tree_scale = jnp.exp(tree_max - top)
    attended = (
        (cache_values * cache_scale[..., None] + tree_values * tree_scale[..., None])
        / (cache_total * cache_scale + tree_total * tree_scale)[..., None]
    ).astype(jnp.bfloat16)
    return attended.reshape(attended.shape[0], attended.shape[1] * attended.shape[2])


def per_device(
    tokens,
    gain_pre,
    w_query,
    w_key,
    w_value,
    w_forget,
    b_forget,
    w_out,
    gain_post,
    key_cache,
    value_cache,
    cum_cache,
    lengths,
    accepted,
    parent,
):
    num_seqs, proposals, model_width = tokens.shape
    kv_rank = lax.axis_index("kv")
    tp_rank = lax.axis_index("tp")
    span = key_cache.shape[1]
    heads_local = key_cache.shape[2]
    head_dim = key_cache.shape[3]
    scale = head_dim ** (-0.5)
    all_rows = num_seqs * proposals
    tok_float = tokens.astype(jnp.float32)
    normed = (
        tok_float
        * lax.rsqrt(jnp.mean(tok_float * tok_float, -1, keepdims=True) + epsilon)
        * gain_pre
    ).astype(jnp.bfloat16)
    flat = normed.reshape(all_rows, model_width)
    weight_rows = w_query.shape[0]
    local_rows = lax.dynamic_slice_in_dim(flat, kv_rank * weight_rows, weight_rows, 1)
    query_part = jnp.dot(local_rows, w_query, preferred_element_type=jnp.float32)
    key_part = jnp.dot(local_rows, w_key, preferred_element_type=jnp.float32)
    value_part = jnp.dot(local_rows, w_value, preferred_element_type=jnp.float32)
    forget_cols = lax.dynamic_slice_in_dim(w_forget, tp_rank * heads_local, heads_local, 1)
    forget_bias = lax.dynamic_slice_in_dim(b_forget, tp_rank * heads_local, heads_local, 0)
    log_forget = jax.nn.log_sigmoid(
        jnp.dot(flat, forget_cols, preferred_element_type=jnp.float32) + forget_bias
    ).reshape(num_seqs, proposals, heads_local)
    ancestors = ancestry(parent, proposals)
    path = jnp.einsum("bij,bjh->bih", ancestors, log_forget, precision=lax.Precision.HIGHEST)
    valid = lengths + accepted
    positions = kv_rank * span + jnp.arange(span, dtype=jnp.int32)
    owner = positions[None, :] == (valid - 1)[:, None]
    last_part = jnp.sum(jnp.where(owner[:, :, None], cum_cache, 0.0), axis=1)
    last_part = jnp.broadcast_to(
        last_part[:, None, :], (num_seqs, proposals, heads_local)
    ).reshape(all_rows, heads_local)
    kv_size = lax.axis_size("kv")
    rows_local = all_rows // kv_size
    own_row = kv_rank * rows_local
    seqs_local = max(1, rows_local // proposals)
    own_seq = own_row // proposals
    rows_each = rows_local // seqs_local
    head_width = heads_local * head_dim
    lanes = -(-3 * heads_local // 128) * 128
    sent = jnp.concatenate(
        [
            query_part.astype(jnp.bfloat16),
            key_part.astype(jnp.bfloat16),
            value_part.astype(jnp.bfloat16),
            pack_lanes(last_part, lanes),
        ],
        axis=1,
    )
    own = jnp.sum(exchange(sent, "kv").astype(jnp.float32), axis=0).astype(jnp.bfloat16)
    full = gather_rows(own, "kv")
    own_last = unpack_lanes(own[:, 3 * head_width :], heads_local)
    last_rows_all = unpack_lanes(full[:, 3 * head_width :], heads_local)
    last_cum = last_rows_all.reshape(num_seqs, proposals, heads_local)[:, 0]
    query = full[:, :head_width].reshape(num_seqs, proposals, heads_local, head_dim)
    key_new = full[:, head_width : 2 * head_width].reshape(
        num_seqs, proposals, heads_local, head_dim
    )
    value_new = full[:, 2 * head_width : 3 * head_width].reshape(
        num_seqs, proposals, heads_local, head_dim
    )
    live = (positions[None, :] < valid[:, None])[:, None, None, :]
    score = (
        jnp.einsum("bihd,bkhd->bihk", query, key_cache, preferred_element_type=jnp.float32) * scale
        + path[..., None]
        - jnp.swapaxes(cum_cache, 1, 2)[:, None]
    )
    block_max = jnp.max(jnp.where(live, score, floor_value), axis=-1)
    weight = jnp.exp(jnp.where(live, score - block_max[..., None], floor_value))
    block_total = jnp.sum(weight, axis=-1)
    block_values = jnp.einsum(
        "bihk,bkhd->bihd",
        weight.astype(jnp.bfloat16),
        value_cache,
        preferred_element_type=jnp.float32,
    )
    has_live = block_total > 0.0
    safe_total = jnp.where(has_live, block_total, 1.0)
    block_mean = (block_values / safe_total[..., None]).astype(jnp.bfloat16)
    block_log = jnp.where(has_live, block_max + jnp.log(safe_total), floor_value)
    blocks_in = exchange(
        jnp.concatenate(
            [
                block_mean.reshape(all_rows, head_width),
                pack_lanes(block_log.reshape(all_rows, heads_local), lanes),
            ],
            axis=1,
        ),
        "kv",
    )
    own_query = own[:, :head_width].reshape(seqs_local, rows_each, heads_local, head_dim)
    own_keys = lax.dynamic_slice_in_dim(key_new, own_seq, seqs_local, 0)
    own_values = lax.dynamic_slice_in_dim(value_new, own_seq, seqs_local, 0)
    seq_path = lax.dynamic_slice_in_dim(path, own_seq, seqs_local, 0)
    own_path = lax.dynamic_slice_in_dim(
        path.reshape(all_rows, heads_local), own_row, rows_local, 0
    ).reshape(seqs_local, rows_each, heads_local)
    own_ancestors = lax.dynamic_slice_in_dim(
        ancestors.reshape(all_rows, proposals), own_row, rows_local, 0
    ).reshape(seqs_local, rows_each, proposals)
    tree_mask = (own_ancestors > 0.5)[:, :, None, :]
    tree_score = (
        jnp.einsum("bihd,bjhd->bihj", own_query, own_keys, preferred_element_type=jnp.float32)
        * scale
        + own_path[..., None]
        - jnp.swapaxes(seq_path, 1, 2)[:, None]
    )
    tree_max = jnp.max(jnp.where(tree_mask, tree_score, floor_value), axis=-1)
    tree_weight = jnp.exp(jnp.where(tree_mask, tree_score - tree_max[..., None], floor_value))
    tree_total = jnp.sum(tree_weight, axis=-1)
    tree_values = jnp.einsum(
        "bihj,bjhd->bihd",
        tree_weight.astype(jnp.bfloat16),
        own_values,
        preferred_element_type=jnp.float32,
    )
    logs_in = unpack_lanes(blocks_in[:, :, head_width:], heads_local)
    cache_max = jnp.max(logs_in, axis=0)
    shares = jnp.exp(logs_in - cache_max[None])
    cache_total = jnp.sum(shares, axis=0)
    cache_values = jnp.sum(
        blocks_in[:, :, :head_width]
        .astype(jnp.float32)
        .reshape(kv_size, rows_local, heads_local, head_dim)
        * shares[..., None],
        axis=0,
    )
    own_attended = finish_rows(
        cache_max,
        cache_total,
        cache_values,
        own_last,
        tree_max.reshape(rows_local, heads_local),
        tree_total.reshape(rows_local, heads_local),
        tree_values.reshape(rows_local, heads_local, head_dim),
    )
    attended = gather_rows(own_attended, "kv")
    mixed_part = jnp.dot(attended, w_out, preferred_element_type=jnp.float32)
    mixed_sum = scatter_columns(mixed_part.astype(jnp.bfloat16), "tp")
    own_squares = jnp.sum(mixed_sum * mixed_sum, axis=1)
    squares = jnp.sum(
        gather_rows(own_squares[None], ("kv", "tp")), axis=0
    )
    mixed = (mixed_sum * lax.rsqrt(squares / model_width + epsilon)[:, None] * gain_post).astype(
        jnp.bfloat16
    )
    mixed = mixed.reshape(num_seqs, proposals, mixed_sum.shape[1])
    relative = positions[None, :] - valid[:, None]
    select = relative[:, :, None] == jnp.arange(proposals, dtype=jnp.int32)[None, None, :]
    written = (relative >= 0) & (relative < proposals)
    placed_keys = jnp.einsum(
        "bkj,bjhd->bkhd", select.astype(jnp.bfloat16), key_new, preferred_element_type=jnp.float32
    ).astype(jnp.bfloat16)
    placed_values = jnp.einsum(
        "bkj,bjhd->bkhd", select.astype(jnp.bfloat16), value_new, preferred_element_type=jnp.float32
    ).astype(jnp.bfloat16)
    key_out = jnp.where(written[:, :, None, None], placed_keys, key_cache)
    value_out = jnp.where(written[:, :, None, None], placed_values, value_cache)
    cum_new = last_cum[:, None, :] + path
    placed_cum = jnp.einsum(
        "bkj,bjh->bkh", select.astype(jnp.float32), cum_new, precision=lax.Precision.HIGHEST
    )
    cum_out = jnp.where(written[:, :, None], placed_cum, cum_cache)
    return (mixed, key_out, value_out, cum_out)


def solution(mesh):
    return jax.shard_map(
        per_device,
        mesh=mesh,
        in_specs=(
            P(),
            P(),
            P("kv", "tp"),
            P("kv", "tp"),
            P("kv", "tp"),
            P(),
            P(),
            P("tp", "kv"),
            P(("kv", "tp")),
            P(None, "kv", "tp", None),
            P(None, "kv", "tp", None),
            P(None, "kv", "tp"),
            P(),
            P(),
            P(),
        ),
        out_specs=(
            P(None, None, ("kv", "tp")),
            P(None, "kv", "tp", None),
            P(None, "kv", "tp", None),
            P(None, "kv", "tp"),
        ),
        check_vma=False,
    )
```

```python
import jax
import jax.numpy as jnp
from jax import lax
from jax.experimental import pallas as pl
from jax.experimental.pallas import tpu as pltpu
from jax.sharding import PartitionSpec as P

epsilon = 1e-06
floor_value = -1e30


def split_float(x):
    high = lax.reduce_precision(x, 8, 7)
    rest = x - high
    middle = lax.reduce_precision(rest, 8, 7)
    low = rest - middle
    return [part.astype(jnp.bfloat16) for part in (high, middle, low)]


def pack_lanes(x, lanes):
    parts = jnp.concatenate(split_float(x), axis=-1)
    return jnp.pad(parts, ((0, 0), (0, lanes - parts.shape[-1])))


def unpack_lanes(packed, count):
    wide = packed.astype(jnp.float32)
    return (
        wide[..., :count] + wide[..., count : 2 * count] + wide[..., 2 * count : 3 * count]
    )


def gather_rows(rows, axis):
    size = lax.axis_size(axis)
    copies = jnp.broadcast_to(rows[None], (size,) + rows.shape)
    return lax.all_to_all(copies, axis, 0, 0, tiled=True).reshape(
        (size * rows.shape[0],) + rows.shape[1:]
    )


def exchange(rows, axis):
    size = lax.axis_size(axis)
    blocks = rows.reshape((size, rows.shape[0] // size) + rows.shape[1:])
    return lax.all_to_all(blocks, axis, 0, 0, tiled=True)


def shifted(block, axis, step):
    size = lax.axis_size(axis)
    return lax.ppermute(block, axis, [(i, (i + step) % size) for i in range(size)])


def fold_of(axis):
    return 2 if lax.axis_size(axis) % 2 == 0 else 1


def fold_sum(rows, axis):
    size = lax.axis_size(axis)
    fold = fold_of(axis)
    groups = size // fold
    rank = lax.axis_index(axis)
    blocks = rows.reshape((groups, fold, rows.shape[0] // size) + rows.shape[1:])
    mine = rank % fold
    half = lax.dynamic_index_in_dim(blocks, mine, 1, False)
    if fold > 1:
        arrived = lax.ppermute(
            lax.dynamic_index_in_dim(blocks, 1 - mine, 1, False),
            axis,
            [(i, i ^ 1) for i in range(size)],
        )
        half = (half.astype(jnp.float32) + arrived.astype(jnp.float32)).astype(rows.dtype)
    group = rank // fold
    total = lax.dynamic_index_in_dim(half, group, 0, False).astype(jnp.float32)
    for step in range(1, groups):
        block = lax.dynamic_index_in_dim(half, (group + step) % groups, 0, False)
        arrived = shifted(block, axis, step * fold)
        total = total + arrived.astype(jnp.float32)
    return total


def fold_gather(rows, axis):
    size = lax.axis_size(axis)
    fold = fold_of(axis)
    groups = size // fold
    rank = lax.axis_index(axis)
    group = rank // fold
    held = jnp.zeros((groups,) + rows.shape, rows.dtype)
    held = lax.dynamic_update_index_in_dim(held, rows, group, 0)
    for step in range(1, groups):
        arrived = shifted(rows, axis, step * fold)
        held = lax.dynamic_update_index_in_dim(
            held, arrived, (group + groups - step) % groups, 0
        )
    if fold == 1:
        return held.reshape((size * rows.shape[0],) + rows.shape[1:])
    other = lax.ppermute(held, axis, [(i, i ^ 1) for i in range(size)])
    even = rank % 2 == 0
    both = jnp.stack([jnp.where(even, held, other), jnp.where(even, other, held)], axis=1)
    return both.reshape((size * rows.shape[0],) + rows.shape[1:])


def scatter_columns(part, axis):
    size = lax.axis_size(axis)
    rank = lax.axis_index(axis)
    width = part.shape[1] // size
    arrived = [
        lax.ppermute(
            lax.dynamic_slice_in_dim(part, ((rank + step) % size) * width, width, 1),
            axis,
            [(i, (i + step) % size) for i in range(size)],
        )
        for step in range(1, size)
    ]
    total = lax.dynamic_slice_in_dim(part, rank * width, width, 1).astype(jnp.float32)
    for block in arrived:
        total = total + block.astype(jnp.float32)
    return total


def write_kernel(starts, key_in, value_in, key_new, value_new, key_out, value_out):
    seqs, span = key_in.shape[:2]
    members = key_new.shape[1]
    key_out[...] = key_in[...]
    value_out[...] = value_in[...]
    for local in range(seqs):
        start = starts[pl.program_id(0) * seqs + local]

        @pl.when((start > -members) & (start < span))
        def _():
            def place(member, carry):
                spot = start + member

                @pl.when((spot >= 0) & (spot < span))
                def _():
                    key_out[local, spot] = key_new[local, member]
                    value_out[local, spot] = value_new[local, member]

                return carry

            lax.fori_loop(0, members, place, 0)


def write_rows(starts, key_cache, value_cache, key_new, value_new):
    num_seqs, span, heads, width = key_cache.shape
    members = key_new.shape[1]
    step = 2 if num_seqs % 2 == 0 else 1
    cache_spec = pl.BlockSpec((step, span, heads, width), lambda s, starts: (s, 0, 0, 0))
    new_spec = pl.BlockSpec((step, members, heads, width), lambda s, starts: (s, 0, 0, 0))
    shape = jax.ShapeDtypeStruct(key_cache.shape, key_cache.dtype)
    return pl.pallas_call(
        write_kernel,
        out_shape=(shape, shape),
        grid_spec=pltpu.PrefetchScalarGridSpec(
            num_scalar_prefetch=1,
            grid=(num_seqs // step,),
            in_specs=[cache_spec, cache_spec, new_spec, new_spec],
            out_specs=(cache_spec, cache_spec),
        ),
        cost_estimate=pl.CostEstimate(
            flops=8 * key_cache.size, bytes_accessed=8 * key_cache.size, transcendentals=0
        ),
    )(starts, key_cache, value_cache, key_new, value_new)


def ancestry(parent_ids, members):
    identity = jnp.eye(members, dtype=jnp.float32)
    parent_hot = (
        parent_ids[:, :, None] == jnp.arange(members, dtype=jnp.int32)[None, None, :]
    ).astype(jnp.float32)
    ancestors = jnp.minimum(identity[None] + parent_hot, 1.0)
    for _ in range(max(1, (members - 1).bit_length())):
        ancestors = jnp.minimum(
            jnp.einsum("bij,bjk->bik", ancestors, ancestors, precision=lax.Precision.HIGHEST), 1.0
        )
    return ancestors


def finish_rows(cache_max, cache_total, cache_values, last_rows, tree_max, tree_total, tree_values):
    shifted = cache_max + last_rows
    top = jnp.maximum(shifted, tree_max)
    cache_scale = jnp.exp(shifted - top)
    tree_scale = jnp.exp(tree_max - top)
    attended = (
        (cache_values * cache_scale[..., None] + tree_values * tree_scale[..., None])
        / (cache_total * cache_scale + tree_total * tree_scale)[..., None]
    ).astype(jnp.bfloat16)
    return attended.reshape(attended.shape[0], attended.shape[1] * attended.shape[2])


def per_device(
    tokens,
    gain_pre,
    w_query,
    w_key,
    w_value,
    w_forget,
    b_forget,
    w_out,
    gain_post,
    key_cache,
    value_cache,
    cum_cache,
    lengths,
    accepted,
    parent,
):
    num_seqs, proposals, model_width = tokens.shape
    kv_rank = lax.axis_index("kv")
    tp_rank = lax.axis_index("tp")
    span = key_cache.shape[1]
    heads_local = key_cache.shape[2]
    head_dim = key_cache.shape[3]
    scale = head_dim ** (-0.5)
    all_rows = num_seqs * proposals
    weight_rows = w_query.shape[0]
    tok_float = tokens.astype(jnp.float32)
    inverse = lax.rsqrt(jnp.mean(tok_float * tok_float, -1, keepdims=True) + epsilon)
    local_first = kv_rank * weight_rows
    local_rows = (
        (
            lax.dynamic_slice_in_dim(tokens, local_first, weight_rows, 2).astype(jnp.float32)
            * inverse
            * lax.dynamic_slice_in_dim(gain_pre, local_first, weight_rows, 0)
        )
        .astype(jnp.bfloat16)
        .reshape(all_rows, weight_rows)
    )
    query_part = jnp.dot(local_rows, w_query, preferred_element_type=jnp.float32)
    kv_size = lax.axis_size("kv")
    rows_local = all_rows // kv_size
    query_in = exchange(query_part.astype(jnp.bfloat16), "kv")
    own_queries = jnp.sum(query_in.astype(jnp.float32), axis=0).astype(jnp.bfloat16)
    query_all = gather_rows(own_queries, "kv")
    flat = (tok_float * inverse * gain_pre).astype(jnp.bfloat16).reshape(all_rows, model_width)
    key_part = jnp.dot(local_rows, w_key, preferred_element_type=jnp.float32)
    value_part = jnp.dot(local_rows, w_value, preferred_element_type=jnp.float32)
    forget_cols = lax.dynamic_slice_in_dim(w_forget, tp_rank * heads_local, heads_local, 1)
    forget_bias = lax.dynamic_slice_in_dim(b_forget, tp_rank * heads_local, heads_local, 0)
    log_forget = jax.nn.log_sigmoid(
        jnp.dot(flat, forget_cols, preferred_element_type=jnp.float32) + forget_bias
    ).reshape(num_seqs, proposals, heads_local)
    ancestors = ancestry(parent, proposals)
    path = jnp.einsum("bij,bjh->bih", ancestors, log_forget, precision=lax.Precision.HIGHEST)
    valid = lengths + accepted
    positions = kv_rank * span + jnp.arange(span, dtype=jnp.int32)
    owner = positions[None, :] == (valid - 1)[:, None]
    last_part = jnp.sum(jnp.where(owner[:, :, None], cum_cache, 0.0), axis=1)
    last_part = jnp.broadcast_to(
        last_part[:, None, :], (num_seqs, proposals, heads_local)
    ).reshape(all_rows, heads_local)
    own_row = kv_rank * rows_local
    seqs_local = max(1, rows_local // proposals)
    own_seq = own_row // proposals
    rows_each = rows_local // seqs_local
    head_width = heads_local * head_dim
    lanes = -(-3 * heads_local // 128) * 128
    sent = jnp.concatenate(
        [
            key_part.astype(jnp.bfloat16),
            value_part.astype(jnp.bfloat16),
            pack_lanes(last_part, lanes),
        ],
        axis=1,
    )
    own = fold_sum(sent, "kv").astype(jnp.bfloat16)
    full = fold_gather(own, "kv")
    own_last = unpack_lanes(own[:, 2 * head_width :], heads_local)
    last_rows_all = unpack_lanes(full[:, 2 * head_width :], heads_local)
    last_cum = last_rows_all.reshape(num_seqs, proposals, heads_local)[:, 0]
    query = query_all.reshape(num_seqs, proposals, heads_local, head_dim)
    key_new = full[:, :head_width].reshape(num_seqs, proposals, heads_local, head_dim)
    value_new = full[:, head_width : 2 * head_width].reshape(
        num_seqs, proposals, heads_local, head_dim
    )
    live = (positions[None, :] < valid[:, None])[:, None, None, :]
    score = (
        jnp.einsum("bihd,bkhd->bihk", query, key_cache, preferred_element_type=jnp.float32) * scale
        + path[..., None]
        - jnp.swapaxes(cum_cache, 1, 2)[:, None]
    )
    block_max = jnp.max(jnp.where(live, score, floor_value), axis=-1)
    weight = jnp.exp(jnp.where(live, score - block_max[..., None], floor_value))
    block_total = jnp.sum(weight, axis=-1)
    block_values = jnp.einsum(
        "bihk,bkhd->bihd",
        weight.astype(jnp.bfloat16),
        value_cache,
        preferred_element_type=jnp.float32,
    )
    has_live = block_total > 0.0
    safe_total = jnp.where(has_live, block_total, 1.0)
    block_mean = (block_values / safe_total[..., None]).astype(jnp.bfloat16)
    block_log = jnp.where(has_live, block_max + jnp.log(safe_total), floor_value)
    blocks_in = exchange(
        jnp.concatenate(
            [
                block_mean.reshape(all_rows, head_width),
                pack_lanes(block_log.reshape(all_rows, heads_local), lanes),
            ],
            axis=1,
        ),
        "kv",
    )
    own_query = own_queries.reshape(seqs_local, rows_each, heads_local, head_dim)
    if rows_local % proposals == 0:
        pair = own[:, : 2 * head_width].reshape(seqs_local, proposals, 2, heads_local, head_dim)
        own_keys = pair[:, :, 0]
        own_values = pair[:, :, 1]
    else:
        own_keys = lax.dynamic_slice_in_dim(key_new, own_seq, seqs_local, 0)
        own_values = lax.dynamic_slice_in_dim(value_new, own_seq, seqs_local, 0)
    seq_path = lax.dynamic_slice_in_dim(path, own_seq, seqs_local, 0)
    own_path = lax.dynamic_slice_in_dim(
        path.reshape(all_rows, heads_local), own_row, rows_local, 0
    ).reshape(seqs_local, rows_each, heads_local)
    own_ancestors = lax.dynamic_slice_in_dim(
        ancestors.reshape(all_rows, proposals), own_row, rows_local, 0
    ).reshape(seqs_local, rows_each, proposals)
    tree_mask = (own_ancestors > 0.5)[:, :, None, :]
    tree_score = (
        jnp.einsum("bihd,bjhd->bihj", own_query, own_keys, preferred_element_type=jnp.float32)
        * scale
        + own_path[..., None]
        - jnp.swapaxes(seq_path, 1, 2)[:, None]
    )
    tree_max = jnp.max(jnp.where(tree_mask, tree_score, floor_value), axis=-1)
    tree_weight = jnp.exp(jnp.where(tree_mask, tree_score - tree_max[..., None], floor_value))
    tree_total = jnp.sum(tree_weight, axis=-1)
    tree_values = jnp.einsum(
        "bihj,bjhd->bihd",
        tree_weight.astype(jnp.bfloat16),
        own_values,
        preferred_element_type=jnp.float32,
    )
    logs_in = unpack_lanes(blocks_in[:, :, head_width:], heads_local)
    cache_max = jnp.max(logs_in, axis=0)
    shares = jnp.exp(logs_in - cache_max[None])
    cache_total = jnp.sum(shares, axis=0)
    cache_values = jnp.sum(
        blocks_in[:, :, :head_width]
        .astype(jnp.float32)
        .reshape(kv_size, rows_local, heads_local, head_dim)
        * shares[..., None],
        axis=0,
    )
    own_attended = finish_rows(
        cache_max,
        cache_total,
        cache_values,
        own_last,
        tree_max.reshape(rows_local, heads_local),
        tree_total.reshape(rows_local, heads_local),
        tree_values.reshape(rows_local, heads_local, head_dim),
    )
    attended = gather_rows(own_attended, "kv")
    mixed_part = jnp.dot(attended, w_out, preferred_element_type=jnp.float32)
    mixed_sum = scatter_columns(mixed_part.astype(jnp.bfloat16), "tp")
    own_squares = jnp.sum(mixed_sum * mixed_sum, axis=1)
    squares = jnp.sum(
        gather_rows(own_squares[None], ("kv", "tp")), axis=0
    )
    mixed = (mixed_sum * lax.rsqrt(squares / model_width + epsilon)[:, None] * gain_post).astype(
        jnp.bfloat16
    )
    mixed = mixed.reshape(num_seqs, proposals, mixed_sum.shape[1])
    relative = positions[None, :] - valid[:, None]
    select = relative[:, :, None] == jnp.arange(proposals, dtype=jnp.int32)[None, None, :]
    written = (relative >= 0) & (relative < proposals)
    key_out, value_out = write_rows(
        valid - kv_rank * span, key_cache, value_cache, key_new, value_new
    )
    cum_new = last_cum[:, None, :] + path
    placed_cum = jnp.einsum(
        "bkj,bjh->bkh", select.astype(jnp.float32), cum_new, precision=lax.Precision.HIGHEST
    )
    cum_out = jnp.where(written[:, :, None], placed_cum, cum_cache)
    return (mixed, key_out, value_out, cum_out)


def solution(mesh):
    return jax.shard_map(
        per_device,
        mesh=mesh,
        in_specs=(
            P(),
            P(),
            P("kv", "tp"),
            P("kv", "tp"),
            P("kv", "tp"),
            P(),
            P(),
            P("tp", "kv"),
            P(("kv", "tp")),
            P(None, "kv", "tp", None),
            P(None, "kv", "tp", None),
            P(None, "kv", "tp"),
            P(),
            P(),
            P(),
        ),
        out_specs=(
            P(None, None, ("kv", "tp")),
            P(None, "kv", "tp", None),
            P(None, "kv", "tp", None),
            P(None, "kv", "tp"),
        ),
        check_vma=False,
    )
```

```python
import jax
import jax.numpy as jnp
from jax import lax
from jax.experimental import pallas as pl
from jax.experimental.layout import Layout, with_layout_constraint
from jax.experimental.pallas import tpu as pltpu
from jax.sharding import PartitionSpec as P

epsilon = 1e-06
floor_value = -1e30


def split_float(x):
    high = lax.reduce_precision(x, 8, 7)
    rest = x - high
    middle = lax.reduce_precision(rest, 8, 7)
    low = rest - middle
    return [part.astype(jnp.bfloat16) for part in (high, middle, low)]


def pack_lanes(x, lanes):
    parts = jnp.concatenate(split_float(x), axis=-1)
    return jnp.pad(parts, ((0, 0), (0, lanes - parts.shape[-1])))


def unpack_lanes(packed, count):
    wide = packed.astype(jnp.float32)
    return (
        wide[..., :count] + wide[..., count : 2 * count] + wide[..., 2 * count : 3 * count]
    )


def gather_rows(rows, axis):
    size = lax.axis_size(axis)
    copies = jnp.broadcast_to(rows[None], (size,) + rows.shape)
    return lax.all_to_all(copies, axis, 0, 0, tiled=True).reshape(
        (size * rows.shape[0],) + rows.shape[1:]
    )


def exchange(rows, axis):
    size = lax.axis_size(axis)
    blocks = rows.reshape((size, rows.shape[0] // size) + rows.shape[1:])
    return lax.all_to_all(blocks, axis, 0, 0, tiled=True)


def shifted(block, axis, step):
    size = lax.axis_size(axis)
    return lax.ppermute(block, axis, [(i, (i + step) % size) for i in range(size)])


def row_major(array):
    return with_layout_constraint(array, Layout(major_to_minor=tuple(range(array.ndim))))


def fold_of(axis):
    return 2 if lax.axis_size(axis) % 2 == 0 else 1


def fold_sum(rows, axis):
    size = lax.axis_size(axis)
    fold = fold_of(axis)
    groups = size // fold
    rank = lax.axis_index(axis)
    blocks = rows.reshape((groups, fold, rows.shape[0] // size) + rows.shape[1:])
    mine = rank % fold
    half = lax.dynamic_index_in_dim(blocks, mine, 1, False)
    if fold > 1:
        arrived = lax.ppermute(
            row_major(lax.dynamic_index_in_dim(blocks, 1 - mine, 1, False)),
            axis,
            [(i, i ^ 1) for i in range(size)],
        )
        half = row_major(
            (half.astype(jnp.float32) + row_major(arrived).astype(jnp.float32)).astype(rows.dtype)
        )
    group = rank // fold
    total = lax.dynamic_index_in_dim(half, group, 0, False).astype(jnp.float32)
    for step in range(1, groups):
        block = row_major(
            lax.dynamic_index_in_dim(half, (group + step) % groups, 0, False)
        )
        arrived = row_major(shifted(block, axis, step * fold))
        total = total + arrived.astype(jnp.float32)
    return total


def fold_gather(rows, axis):
    size = lax.axis_size(axis)
    fold = fold_of(axis)
    groups = size // fold
    rank = lax.axis_index(axis)
    group = rank // fold
    held = jnp.zeros((groups,) + rows.shape, rows.dtype)
    held = lax.dynamic_update_index_in_dim(held, rows, group, 0)
    for step in range(1, groups):
        arrived = row_major(shifted(rows, axis, step * fold))
        held = lax.dynamic_update_index_in_dim(
            held, arrived, (group + groups - step) % groups, 0
        )
    if fold == 1:
        return held.reshape((size * rows.shape[0],) + rows.shape[1:])
    held = row_major(held)
    other = row_major(lax.ppermute(held, axis, [(i, i ^ 1) for i in range(size)]))
    even = rank % 2 == 0
    both = jnp.stack([jnp.where(even, held, other), jnp.where(even, other, held)], axis=1)
    return both.reshape((size * rows.shape[0],) + rows.shape[1:])


def scatter_columns(part, axis):
    size = lax.axis_size(axis)
    rank = lax.axis_index(axis)
    width = part.shape[1] // size
    arrived = [
        lax.ppermute(
            lax.dynamic_slice_in_dim(part, ((rank + step) % size) * width, width, 1),
            axis,
            [(i, (i + step) % size) for i in range(size)],
        )
        for step in range(1, size)
    ]
    total = lax.dynamic_slice_in_dim(part, rank * width, width, 1).astype(jnp.float32)
    for block in arrived:
        total = total + block.astype(jnp.float32)
    return total


def write_kernel(starts, cache, new, out, held, in_sems, out_sems):
    seqs, span = cache.shape[:2]
    members = new.shape[1]

    def arriving(seq):
        return pltpu.make_async_copy(cache.at[seq], held.at[seq], in_sems.at[seq])

    def leaving(seq):
        return pltpu.make_async_copy(held.at[seq], out.at[seq], out_sems.at[seq])

    def begin(seq, carry):
        arriving(seq).start()
        return carry

    def patch(seq, carry):
        arriving(seq).wait()
        start = starts[seq]

        @pl.when((start > -members) & (start < span))
        def _():
            for member in range(members):
                spot = start + member

                @pl.when((spot >= 0) & (spot < span))
                def _():
                    held[seq, spot] = new[seq, member]

        leaving(seq).start()
        return carry

    def finish(seq, carry):
        leaving(seq).wait()
        return carry

    lax.fori_loop(0, seqs, begin, 0)
    lax.fori_loop(0, seqs, patch, 0)
    lax.fori_loop(0, seqs, finish, 0)


def write_rows(starts, cache, new):
    num_seqs = cache.shape[0]
    return pl.pallas_call(
        write_kernel,
        out_shape=jax.ShapeDtypeStruct(cache.shape, cache.dtype),
        in_specs=[
            pl.BlockSpec(memory_space=pltpu.SMEM),
            pl.BlockSpec(memory_space=pl.ANY),
            pl.BlockSpec(memory_space=pltpu.VMEM),
        ],
        out_specs=pl.BlockSpec(memory_space=pl.ANY),
        scratch_shapes=[
            pltpu.VMEM(cache.shape, cache.dtype),
            pltpu.SemaphoreType.DMA((num_seqs,)),
            pltpu.SemaphoreType.DMA((num_seqs,)),
        ],
        cost_estimate=pl.CostEstimate(
            flops=8 * cache.size, bytes_accessed=4 * cache.size, transcendentals=0
        ),
    )(starts, cache, new)


def ancestry(parent_ids, members):
    identity = jnp.eye(members, dtype=jnp.float32)
    parent_hot = (
        parent_ids[:, :, None] == jnp.arange(members, dtype=jnp.int32)[None, None, :]
    ).astype(jnp.float32)
    ancestors = jnp.minimum(identity[None] + parent_hot, 1.0)
    for _ in range(max(1, (members - 1).bit_length())):
        ancestors = jnp.minimum(
            jnp.einsum("bij,bjk->bik", ancestors, ancestors, precision=lax.Precision.HIGHEST), 1.0
        )
    return ancestors


def finish_rows(cache_max, cache_total, cache_values, last_rows, tree_max, tree_total, tree_values):
    shifted = cache_max + last_rows
    top = jnp.maximum(shifted, tree_max)
    cache_scale = jnp.exp(shifted - top)
    tree_scale = jnp.exp(tree_max - top)
    attended = (
        (cache_values * cache_scale[..., None] + tree_values * tree_scale[..., None])
        / (cache_total * cache_scale + tree_total * tree_scale)[..., None]
    ).astype(jnp.bfloat16)
    return attended.reshape(attended.shape[0], attended.shape[1] * attended.shape[2])


def per_device(
    tokens,
    gain_pre,
    w_query,
    w_key,
    w_value,
    w_forget,
    b_forget,
    w_out,
    gain_post,
    key_cache,
    value_cache,
    cum_cache,
    lengths,
    accepted,
    parent,
):
    num_seqs, proposals, model_width = tokens.shape
    kv_rank = lax.axis_index("kv")
    tp_rank = lax.axis_index("tp")
    span = key_cache.shape[1]
    heads_local = key_cache.shape[2]
    head_dim = key_cache.shape[3]
    scale = head_dim ** (-0.5)
    all_rows = num_seqs * proposals
    weight_rows = w_query.shape[0]
    tok_float = tokens.astype(jnp.float32)
    inverse = lax.rsqrt(jnp.mean(tok_float * tok_float, -1, keepdims=True) + epsilon)
    local_first = kv_rank * weight_rows
    local_rows = (
        (
            lax.dynamic_slice_in_dim(tokens, local_first, weight_rows, 2).astype(jnp.float32)
            * inverse
            * lax.dynamic_slice_in_dim(gain_pre, local_first, weight_rows, 0)
        )
        .astype(jnp.bfloat16)
        .reshape(all_rows, weight_rows)
    )
    query_part = jnp.dot(local_rows, w_query, preferred_element_type=jnp.float32)
    kv_size = lax.axis_size("kv")
    rows_local = all_rows // kv_size
    query_in = exchange(query_part.astype(jnp.bfloat16), "kv")
    own_queries = jnp.sum(query_in.astype(jnp.float32), axis=0).astype(jnp.bfloat16)
    query_all = gather_rows(own_queries, "kv")
    flat = (tok_float * inverse * gain_pre).astype(jnp.bfloat16).reshape(all_rows, model_width)
    key_part = jnp.dot(local_rows, w_key, preferred_element_type=jnp.float32)
    value_part = jnp.dot(local_rows, w_value, preferred_element_type=jnp.float32)
    forget_cols = lax.dynamic_slice_in_dim(w_forget, tp_rank * heads_local, heads_local, 1)
    forget_bias = lax.dynamic_slice_in_dim(b_forget, tp_rank * heads_local, heads_local, 0)
    log_forget = jax.nn.log_sigmoid(
        jnp.dot(flat, forget_cols, preferred_element_type=jnp.float32) + forget_bias
    ).reshape(num_seqs, proposals, heads_local)
    ancestors = ancestry(parent, proposals)
    path = jnp.einsum("bij,bjh->bih", ancestors, log_forget, precision=lax.Precision.HIGHEST)
    valid = lengths + accepted
    positions = kv_rank * span + jnp.arange(span, dtype=jnp.int32)
    owner = positions[None, :] == (valid - 1)[:, None]
    last_part = jnp.sum(jnp.where(owner[:, :, None], cum_cache, 0.0), axis=1)
    last_part = jnp.broadcast_to(
        last_part[:, None, :], (num_seqs, proposals, heads_local)
    ).reshape(all_rows, heads_local)
    own_row = kv_rank * rows_local
    seqs_local = max(1, rows_local // proposals)
    own_seq = own_row // proposals
    rows_each = rows_local // seqs_local
    head_width = heads_local * head_dim
    lanes = -(-3 * heads_local // 128) * 128
    sent = jnp.concatenate(
        [
            key_part.astype(jnp.bfloat16),
            value_part.astype(jnp.bfloat16),
            pack_lanes(last_part, lanes),
        ],
        axis=1,
    )
    own = row_major(fold_sum(row_major(sent), "kv").astype(jnp.bfloat16))
    full = row_major(fold_gather(own, "kv"))
    own_last = unpack_lanes(own[:, 2 * head_width :], heads_local)
    last_rows_all = unpack_lanes(full[:, 2 * head_width :], heads_local)
    last_cum = last_rows_all.reshape(num_seqs, proposals, heads_local)[:, 0]
    query = query_all.reshape(num_seqs, proposals, heads_local, head_dim)
    key_new = full[:, :head_width].reshape(num_seqs, proposals, heads_local, head_dim)
    value_new = full[:, head_width : 2 * head_width].reshape(
        num_seqs, proposals, heads_local, head_dim
    )
    live = (positions[None, :] < valid[:, None])[:, None, None, :]
    score = (
        jnp.einsum("bihd,bkhd->bihk", query, key_cache, preferred_element_type=jnp.float32) * scale
        - jnp.swapaxes(cum_cache, 1, 2)[:, None]
    )
    block_max = jnp.max(jnp.where(live, score, floor_value), axis=-1)
    weight = jnp.exp(jnp.where(live, score - block_max[..., None], floor_value))
    block_total = jnp.sum(weight, axis=-1)
    block_values = jnp.einsum(
        "bihk,bkhd->bihd",
        weight.astype(jnp.bfloat16),
        value_cache,
        preferred_element_type=jnp.float32,
    )
    has_live = block_total > 0.0
    safe_total = jnp.where(has_live, block_total, 1.0)
    block_mean = (block_values / safe_total[..., None]).astype(jnp.bfloat16)
    block_log = jnp.where(has_live, block_max + jnp.log(safe_total), floor_value)
    blocks_in = exchange(
        jnp.concatenate(
            [
                block_mean.reshape(all_rows, head_width),
                pack_lanes(block_log.reshape(all_rows, heads_local), lanes),
            ],
            axis=1,
        ),
        "kv",
    )
    own_query = own_queries.reshape(seqs_local, rows_each, heads_local, head_dim)
    if rows_local % proposals == 0:
        pair = own[:, : 2 * head_width].reshape(seqs_local, proposals, 2, heads_local, head_dim)
        own_keys = pair[:, :, 0]
        own_values = pair[:, :, 1]
    else:
        own_keys = lax.dynamic_slice_in_dim(key_new, own_seq, seqs_local, 0)
        own_values = lax.dynamic_slice_in_dim(value_new, own_seq, seqs_local, 0)
    seq_path = lax.dynamic_slice_in_dim(path, own_seq, seqs_local, 0)
    own_path = lax.dynamic_slice_in_dim(
        path.reshape(all_rows, heads_local), own_row, rows_local, 0
    ).reshape(seqs_local, rows_each, heads_local)
    own_ancestors = lax.dynamic_slice_in_dim(
        ancestors.reshape(all_rows, proposals), own_row, rows_local, 0
    ).reshape(seqs_local, rows_each, proposals)
    tree_mask = (own_ancestors > 0.5)[:, :, None, :]
    tree_score = (
        jnp.einsum("bihd,bjhd->bihj", own_query, own_keys, preferred_element_type=jnp.float32)
        * scale
        + own_path[..., None]
        - jnp.swapaxes(seq_path, 1, 2)[:, None]
    )
    tree_max = jnp.max(jnp.where(tree_mask, tree_score, floor_value), axis=-1)
    tree_weight = jnp.exp(jnp.where(tree_mask, tree_score - tree_max[..., None], floor_value))
    tree_total = jnp.sum(tree_weight, axis=-1)
    tree_values = jnp.einsum(
        "bihj,bjhd->bihd",
        tree_weight.astype(jnp.bfloat16),
        own_values,
        preferred_element_type=jnp.float32,
    )
    logs_in = unpack_lanes(blocks_in[:, :, head_width:], heads_local)
    row_max = jnp.max(logs_in, axis=0)
    shares = jnp.exp(logs_in - row_max[None])
    cache_max = row_max + own_path.reshape(rows_local, heads_local)
    cache_total = jnp.sum(shares, axis=0)
    cache_values = jnp.sum(
        blocks_in[:, :, :head_width]
        .astype(jnp.float32)
        .reshape(kv_size, rows_local, heads_local, head_dim)
        * shares[..., None],
        axis=0,
    )
    own_attended = finish_rows(
        cache_max,
        cache_total,
        cache_values,
        own_last,
        tree_max.reshape(rows_local, heads_local),
        tree_total.reshape(rows_local, heads_local),
        tree_values.reshape(rows_local, heads_local, head_dim),
    )
    attended = gather_rows(own_attended, "kv")
    mixed_part = jnp.dot(attended, w_out, preferred_element_type=jnp.float32)
    mixed_sum = scatter_columns(mixed_part.astype(jnp.bfloat16), "tp")
    own_squares = jnp.sum(mixed_sum * mixed_sum, axis=1)
    squares_in = gather_rows(own_squares[None], ("kv", "tp"))
    squares = jnp.sum(squares_in, axis=0)
    mixed = (mixed_sum * lax.rsqrt(squares / model_width + epsilon)[:, None] * gain_post).astype(
        jnp.bfloat16
    )
    mixed = mixed.reshape(num_seqs, proposals, mixed_sum.shape[1])
    relative = positions[None, :] - valid[:, None]
    select = relative[:, :, None] == jnp.arange(proposals, dtype=jnp.int32)[None, None, :]
    written = (relative >= 0) & (relative < proposals)
    starts = valid - kv_rank * span
    key_out = write_rows(starts, key_cache, key_new)
    value_out = write_rows(starts, value_cache, value_new)
    cum_new = last_cum[:, None, :] + path
    placed_cum = jnp.einsum(
        "bkj,bjh->bkh", select.astype(jnp.float32), cum_new, precision=lax.Precision.HIGHEST
    )
    cum_out = jnp.where(written[:, :, None], placed_cum, cum_cache)
    return (mixed, key_out, value_out, cum_out)


def solution(mesh):
    return jax.shard_map(
        per_device,
        mesh=mesh,
        in_specs=(
            P(),
            P(),
            P("kv", "tp"),
            P("kv", "tp"),
            P("kv", "tp"),
            P(),
            P(),
            P("tp", "kv"),
            P(("kv", "tp")),
            P(None, "kv", "tp", None),
            P(None, "kv", "tp", None),
            P(None, "kv", "tp"),
            P(),
            P(),
            P(),
        ),
        out_specs=(
            P(None, None, ("kv", "tp")),
            P(None, "kv", "tp", None),
            P(None, "kv", "tp", None),
            P(None, "kv", "tp"),
        ),
        check_vma=False,
    )
```
